32 devices in a mesh: grp: 2 (over x), ra: 4 (over z), cb: 4 (over y, core).
Axes of the slice: x: 2, y: 2, z: 4, core: 2. Of those that a mesh axis runs over, the one named last changes fastest.
Arguments:
- tokens: bfloat16 [256, 4096], P('grp', 'ra'), parts along dimension 0, may hold values from -30 to 30
- in_gain: float32 [4096], P('ra'), may hold values from 0.1 to 1.9
- gate_weight: float32 [4096, 11264], P('ra', 'cb'), may hold values from -0.09375 to 0.09375
- gate_scale: float32 [11264], P('cb'), may hold values from 0.3 to 3
- up_weight: float32 [4096, 11264], P('ra', 'cb'), may hold values from -0.09375 to 0.09375
- up_scale: float32 [11264], P('cb'), may hold values from 0.3 to 3
- down_weight: float32 [11264, 4096], P('cb', 'ra'), may hold values from -0.0546875 to 0.0546875
- down_scale: float32 [4096], P('ra'), may hold values from 0.3 to 3
- out_gain: float32 [4096], P('ra'), may hold values from 0.1 to 1.9
Outputs:
- result: bfloat16 [256, 4096], P('grp', 'ra'), parts along dimension 0
The draws below stay inside these ranges and needn't reach their ends.
There are 2 independent parts, one for each index of `grp`. The reference program is written for one: setup_inputs(seed, part) draws one part's arguments, and reference() takes and returns one part's arrays. A program takes and returns all parts, laid end to end along the dimension named above; an argument that names none is the same for every part. Nothing has to cross between parts.
All inputs are finite; a program needn't handle non-finite values.
Results may differ from the reference program's by a relative error of at most 0.008.
Values may be sent and summed in bfloat16 or wider, within the bound.
A program may use at most 64 MiB of HBM per device.

```python
import math
import jax
import jax.numpy as jnp
from jax import lax

D = 4096
FF = 11264
TOK = 128


def draw_tokens(key, part):
    keys = jax.random.split(jax.random.fold_in(key, 11), 2)
    column = jnp.exp(math.log(10.0) * jnp.arange(D, dtype=jnp.float32) / (D - 1))
    rows = jnp.exp(jax.random.uniform(keys[0], (TOK, 1), jnp.float32, 0.0, math.log(10.0)))
    base = jax.random.normal(keys[1], (TOK, D), jnp.float32)
    values = base * rows * column[None, :]
    values = values / jnp.sqrt(jnp.mean(values * values))
    return jnp.clip(values, -30.0, 30.0).astype(jnp.bfloat16)


def levels(key, dims, cuts, low, high):
    gain, own = 1.0, jax.random.fold_in(key, 6)
    for axis_at, blocks in cuts:
        draws = jnp.exp(jax.random.uniform(jax.random.fold_in(own, axis_at), (blocks,), jnp.float32, low / len(cuts), high / len(cuts)))
        gain = gain * jnp.repeat(draws, dims[axis_at] // blocks).reshape([-1 if axis == axis_at else 1 for axis in range(len(dims))])
    return gain


def bell_draw(rng, extent, spread, most, pieces=(), kind=jnp.bfloat16):
    gain = levels(rng, extent, pieces, -0.22, 0.18) if pieces else 1.0
    drawn = jax.random.normal(rng, extent, jnp.float32) * spread * gain
    return jnp.minimum(jnp.maximum(drawn, -most), most).astype(kind)


def setup_inputs(seed: int = 0, part: int = 0) -> dict:
    arg_keys = jax.random.split(jax.random.key(seed), 10)
    own_keys = jax.random.split(jax.random.fold_in(arg_keys[9], part), 10)
    return {
        "tokens": draw_tokens(jax.random.fold_in(jax.random.fold_in(arg_keys[9], part), 71), part),
        "in_gain": jnp.clip(1.0 + 0.18 * jax.random.normal(arg_keys[1], (D,), jnp.float32), 0.1, 1.9),
        "gate_weight": bell_draw(arg_keys[2], (D, FF), D ** -0.5, 0.09375, ((0, 4), (1, 4)), jnp.float32),
        "gate_scale": jnp.clip(jnp.exp(math.log(3.0) - 2.3025851 * jax.random.uniform(arg_keys[3], (FF,), jnp.float32) ** levels(arg_keys[3], (FF,), ((0, 4),), -0.2, 0.2)), 0.3, 3.0),
        "up_weight": bell_draw(arg_keys[4], (D, FF), D ** -0.5, 0.09375, ((0, 4), (1, 4)), jnp.float32),
        "up_scale": jnp.clip(jnp.exp(math.log(3.0) - 2.3025851 * jax.random.uniform(arg_keys[5], (FF,), jnp.float32) ** levels(arg_keys[5], (FF,), ((0, 4),), -0.2, 0.2)), 0.3, 3.0),
        "down_weight": bell_draw(arg_keys[6], (FF, D), FF ** -0.5, 0.0546875, ((0, 4), (1, 4)), jnp.float32),
        "down_scale": jnp.clip(jnp.exp(math.log(3.0) - 2.3025851 * jax.random.uniform(arg_keys[7], (D,), jnp.float32) ** levels(arg_keys[7], (D,), ((0, 4),), -0.2, 0.2)), 0.3, 3.0),
        "out_gain": jnp.clip(1.0 + 0.18 * jax.random.normal(arg_keys[8], (D,), jnp.float32), 0.1, 1.9),
    }


EPSILON = 1e-06
RESIDUAL = 0.5

def reference(tokens, in_gain, gate_weight, gate_scale, up_weight, up_scale, down_weight, down_scale, out_gain):
    tok_float = tokens.astype(jnp.float32)
    inv_rows = lax.rsqrt(lax.optimization_barrier(jnp.mean(tok_float * tok_float, axis=1, keepdims=True)) + EPSILON)
    scaled = (tok_float * in_gain[None, :]).astype(jnp.bfloat16)
    gate_full = jnp.dot(scaled, gate_weight.astype(jnp.bfloat16), preferred_element_type=jnp.float32) * inv_rows * gate_scale[None, :]
    up_full = jnp.dot(scaled, up_weight.astype(jnp.bfloat16), preferred_element_type=jnp.float32) * inv_rows * up_scale[None, :]
    hidden = (jax.nn.silu(gate_full) * up_full).astype(jnp.bfloat16)
    down_full = jnp.dot(hidden, down_weight.astype(jnp.bfloat16), preferred_element_type=jnp.float32)
    mixed_rows = RESIDUAL * tok_float + down_full * down_scale[None, :]
    inv_out = lax.rsqrt(lax.optimization_barrier(jnp.mean(mixed_rows * mixed_rows, axis=1, keepdims=True)) + EPSILON)
    return (mixed_rows * inv_out * out_gain[None, :]).astype(jnp.bfloat16)
```

```python
import functools
import jax
import jax.numpy as jnp
from jax import lax
from jax.experimental import pallas as pl
from jax.experimental.pallas import tpu as pltpu
from jax.sharding import PartitionSpec as P

EPSILON = 1e-06
RESIDUAL = 0.5


def local(
    tokens, in_gain, gate_weight, gate_scale, up_weight, up_scale, down_weight, down_scale, out_gain
):
    tok_float = tokens.astype(jnp.float32)
    local_squares = jnp.sum(tok_float * tok_float, axis=1)
    scaled = (tok_float * in_gain[None, :]).astype(jnp.bfloat16)
    gate_part = jnp.dot(
        scaled, gate_weight.astype(jnp.bfloat16), preferred_element_type=jnp.float32
    )
    up_part = jnp.dot(scaled, up_weight.astype(jnp.bfloat16), preferred_element_type=jnp.float32)
    features = tokens.shape[1] * lax.axis_size("ra")
    gate_sum, up_sum, share_squares = (
        lax.psum_scatter(gate_part, "ra", scatter_dimension=0, tiled=True),
        lax.psum_scatter(up_part, "ra", scatter_dimension=0, tiled=True),
        lax.psum_scatter(local_squares, "ra", scatter_dimension=0, tiled=True),
    )
    inv_rows = lax.rsqrt(share_squares / features + EPSILON)[:, None]
    gate_share = gate_sum * inv_rows * gate_scale[None, :]
    up_share = up_sum * inv_rows * up_scale[None, :]
    hidden_share = (jax.nn.silu(gate_share) * up_share).astype(jnp.bfloat16)
    hidden = lax.all_gather(hidden_share, "ra", axis=0, tiled=True)
    down_part = jnp.dot(
        hidden, down_weight.astype(jnp.bfloat16), preferred_element_type=jnp.float32
    )
    down_full = lax.psum(down_part, "cb")
    mixed_rows = RESIDUAL * tok_float + down_full * down_scale[None, :]
    out_total = lax.psum(jnp.sum(mixed_rows * mixed_rows, axis=1), "ra")
    inv_out = lax.rsqrt(out_total / features + EPSILON)[:, None]
    return (mixed_rows * inv_out * out_gain[None, :]).astype(jnp.bfloat16)


MESH = pl.DeviceIdType.MESH
WIDTH = 256
SUB = 128
AHEAD = 3
RS_LAG = ((22, 8, 4, 0), (0, 3, 7, 22))
AG_LAG = ((0, 25, 32, 44), (44, 32, 29, 0))
OWN_SEND = (45, 37, 41, 45)
OWN_PASS = (47, 39, 43, 47)
STEPS = 56


def pick(z, values):
    out = jnp.int32(values[0])
    for i, value in enumerate(values[1:], 1):
        out = lax.select(z == i, jnp.int32(value), out)
    return out


def kernel(
    n,
    tok_hbm, gain_hbm, gate_hbm, gscale_hbm, up_hbm, uscale_hbm, down_hbm, dscale_hbm, ogain_hbm,
    out_ref,
    tok, gain, gate, gscale, up, uscale, down, dscale, ogain,
    scaled, part, sent, got, hidden, acc, spread, sq_own, sq_sent, sq_got, inv,
    mate_sent, mate_got, y_sent, y_got, mixed, mixed_got, out_all,
    small_sem, gate_sem, up_sem, down_sem, rs_send, rs_recv, ag_send, ag_recv,
    sq_send, sq_recv, mate_sem, y_sem, mix_sem, out_send, out_recv,
):
    blocks, half = gate.shape[0], tok.shape[0] // 2
    chunks = part.shape[0]
    per = chunks // blocks
    rows = 2 * half
    wide = tok.shape[1] // 2
    features = tok.shape[1] * n
    z, cb = lax.axis_index("ra"), lax.axis_index("cb")
    core = lax.rem(cb, 2)
    mate = cb + 1 - 2 * core
    across = lax.rem(cb + 2, 4)
    right, left = lax.rem(z + 1, n), lax.rem(z + n - 1, n)
    own_side = (z >= n // 2).astype(jnp.int32)
    mine = pl.ds(pl.multiple_of(core * wide, wide), wide)
    theirs = pl.ds(pl.multiple_of((1 - core) * wide, wide), wide)

    smalls = [
        pltpu.make_async_copy(src, dst, small_sem.at[i])
        for i, (src, dst) in enumerate([
            (tok_hbm, tok), (gain_hbm, gain), (gscale_hbm, gscale),
            (uscale_hbm, uscale), (dscale_hbm, dscale), (ogain_hbm, ogain),
        ])
    ]

    def gate_copy(k):
        cols = pl.ds(pl.multiple_of(k * WIDTH, WIDTH), WIDTH)
        return pltpu.make_async_copy(gate_hbm.at[:, cols], gate.at[k], gate_sem.at[k])

    def up_copy(k):
        cols = pl.ds(pl.multiple_of(k * WIDTH, WIDTH), WIDTH)
        return pltpu.make_async_copy(up_hbm.at[:, cols], up.at[k], up_sem.at[k])

    def down_copy(k):
        at = pl.ds(pl.multiple_of(k * WIDTH, WIDTH), WIDTH)
        return pltpu.make_async_copy(down_hbm.at[at, :], down.at[k], down_sem.at[k])

    for copy in smalls[:2]:
        copy.start()
    for k in range(min(AHEAD, blocks)):
        gate_copy(k).start()
        up_copy(k).start()
    for copy in smalls[2:]:
        copy.start()

    barrier = pltpu.get_barrier_semaphore()

    @pl.when(z > 0)
    def _():
        pl.semaphore_signal(barrier, inc=1, device_id={"ra": left}, device_id_type=MESH)

    @pl.when(z < n - 1)
    def _():
        pl.semaphore_signal(barrier, inc=1, device_id={"ra": right}, device_id_type=MESH)

    for who in (mate, across):
        pl.semaphore_signal(barrier, inc=1, device_id={"cb": who}, device_id_type=MESH)

    for copy in smalls[:2]:
        copy.wait()
    tok_float = tok[...].astype(jnp.float32)
    scaled[...] = (tok_float * gain[...]).astype(jnp.bfloat16)
    def sq_copy(side):
        return pltpu.make_async_remote_copy(
            sq_sent.at[side], sq_got.at[side], sq_send.at[side], sq_recv.at[side],
            device_id={"ra": right if side else left}, device_id_type=MESH,
        )

    def rs_copy(j, side):
        return pltpu.make_async_remote_copy(
            sent.at[side, j], got.at[side, j], rs_send.at[side, j], rs_recv.at[side, j],
            device_id={"ra": right if side else left}, device_id_type=MESH,
        )

    def ag_copy(j, side):
        ref = hidden.at[side, j]
        return pltpu.make_async_remote_copy(
            ref, ref, ag_send.at[side, j], ag_recv.at[side, j],
            device_id={"ra": left if side else right}, device_id_type=MESH,
        )

    def rows_of(side):
        return pl.ds(side * half, half)

    def rs_step(s, side):
        place = z if side else n - 1 - z
        j = s - pick(z, RS_LAG[side])

        @pl.when((j >= 0) & (j < chunks) & (place > 0))
        def _():
            @pl.when(place < n - 1)
            def _():
                @pl.when(j == 0)
                def _():
                    sq_copy(side).wait_recv()
                    sq_sent[side] = sq_own[...] + sq_got[side]
                    sq_copy(side).start()

                rs_copy(j, side).wait_recv()
                sent[side, j] = (part[j, rows_of(side)] + got[side, j].astype(jnp.float32)).astype(jnp.bfloat16)
                rs_copy(j, side).start()

            @pl.when(place == n - 1)
            def _():
                @pl.when(j == 0)
                def _():
                    sq_copy(side).wait_recv()
                    total = sq_own[...] + sq_got[side]
                    spread[...] = jnp.broadcast_to(total[:1], (128, 128)).T
                    inv[...] = lax.rsqrt(spread[...] / features + EPSILON)

                rs_copy(j, side).wait_recv()
                scale = inv[rows_of(side)]
                total = part[j, rows_of(side)] + got[side, j].astype(jnp.float32)
                gate_share = total[:, :SUB] * scale * gscale[pl.ds(j, 1)]
                up_share = total[:, SUB:] * scale * uscale[pl.ds(j, 1)]
                hidden[side, j] = (jax.nn.silu(gate_share) * up_share).astype(jnp.bfloat16)
                ag_copy(j, side).start()

    def ag_step(s, side, i):
        place = n - 1 - z if side else z
        j = per * (s - pick(z, AG_LAG[side])) + i

        @pl.when((j >= 0) & (j < chunks) & (place > 0))
        def _():
            ag_copy(j, side).wait_recv()

            @pl.when(place < n - 1)
            def _():
                ag_copy(j, side).start()

    def down_step(s, side):
        place = n - 1 - z if side else z
        since = s - pick(z, RS_LAG[side])
        k = lax.select(place > 0, s - pick(z, AG_LAG[side]), since // per)

        @pl.when((k >= 0) & (k < blocks) & ((place > 0) | (lax.rem(since, per) == per - 1)))
        def _():
            @pl.when(own_side == side)
            def _():
                down_copy(k).wait()

            units = jnp.concatenate([hidden[side, per * k + i] for i in range(per)], axis=1)
            weights = down[k].astype(jnp.bfloat16)
            acc[side] += jnp.dot(units, weights, preferred_element_type=jnp.float32)

    def mate_copy(side):
        return pltpu.make_async_remote_copy(
            mate_sent.at[side], mate_got.at[side], mate_sem.at[0, side], mate_sem.at[1, side],
            device_id={"cb": mate}, device_id_type=MESH,
        )

    def y_copy(side):
        return pltpu.make_async_remote_copy(
            y_sent.at[side], y_got.at[side], y_sem.at[0, side], y_sem.at[1, side],
            device_id={"cb": across}, device_id_type=MESH,
        )

    def mix_copy(side):
        at = rows_of(side)
        return pltpu.make_async_remote_copy(
            mixed.at[at], mixed_got.at[at], mix_sem.at[0, side], mix_sem.at[1, side],
            device_id={"cb": mate}, device_id_type=MESH,
        )

    def mate_start(side):
        mate_sent[side] = acc[side, :, theirs].astype(jnp.bfloat16)
        mate_copy(side).start()

    def y_start(side):
        mate_copy(side).wait_recv()
        y_sent[side] = (acc[side, :, mine] + mate_got[side].astype(jnp.float32)).astype(jnp.bfloat16)
        y_copy(side).start()

    def mix_start(side):
        y_copy(side).wait_recv()
        at = rows_of(side)
        summed = y_sent[side].astype(jnp.float32) + y_got[side].astype(jnp.float32)
        value = RESIDUAL * tok[at, mine].astype(jnp.float32) + summed * dscale[:, mine]
        mixed[at] = value
        spread[at] = jnp.broadcast_to(jnp.sum(value * value, axis=1, keepdims=True), (half, 128))

    def step(s, carry):
        @pl.when((s < chunks) & (lax.rem(s, per) == 0))
        def _():
            k = s // per

            def store(product, offset):
                for i in range(per):
                    part[s + i, :, offset:offset + SUB] = product[:, SUB * i:SUB * (i + 1)]

            gate_copy(k).wait()
            store(jnp.dot(scaled[...], gate[k].astype(jnp.bfloat16), preferred_element_type=jnp.float32), 0)
            up_copy(k).wait()

            @pl.when(k + AHEAD < blocks)
            def _():
                gate_copy(k + AHEAD).start()
                up_copy(k + AHEAD).start()

            down_copy(k).start()
            store(jnp.dot(scaled[...], up[k].astype(jnp.bfloat16), preferred_element_type=jnp.float32), SUB)
            @pl.when(k == 0)
            def _():
                tok_float = tok[...].astype(jnp.float32)
                squares = jnp.sum(tok_float * tok_float, axis=1, keepdims=True)
                spread[...] = jnp.broadcast_to(squares, (rows, 128))
                sq_own[...] = spread[...].T[:8]
                pl.semaphore_wait(barrier, 2 + (z > 0).astype(jnp.int32) + (z < n - 1).astype(jnp.int32))

            for side in range(2):
                @pl.when(z == (0 if side else n - 1))
                def _():
                    for i in range(per):
                        sent[side, s + i] = part[s + i, rows_of(side)].astype(jnp.bfloat16)
                        rs_copy(s + i, side).start()

                    @pl.when(k == 0)
                    def _():
                        sq_sent[side] = sq_own[...]
                        sq_copy(side).start()

        @pl.when(s == 0)
        def _():
            for copy in smalls[2:]:
                copy.wait()
            for side in range(2):
                acc[side] = jnp.zeros_like(acc[side])

        for side in (1, 0):
            rs_step(s, side)
        for i in range(per):
            for side in range(2):
                ag_step(s, side, i)
        for side in range(2):
            down_step(s, side)
        for side in range(2):
            @pl.when(own_side == side)
            def _():
                @pl.when(s == pick(z, OWN_SEND))
                def _():
                    mate_start(side)

                @pl.when(s == pick(z, OWN_PASS))
                def _():
                    y_start(side)

        return carry

    lax.fori_loop(0, STEPS, step, 0)

    for side in range(2):
        @pl.when(own_side != side)
        def _():
            mate_start(side)
            mix_start(1 - side)
            mix_copy(1 - side).start()
            y_start(side)
            mix_start(side)

    at = 2 * z + core
    out_all[at] = spread[...].T[:8]

    def out_copies(arriving):
        made = []
        for step in range(n):
            for other in range(2):
                if step or other:
                    slot = 2 * step + other - 1
                    source = 2 * lax.rem(z + n - step, n) + (1 - core if other else core)
                    ref = out_all.at[source if arriving else at]
                    made.append(pltpu.make_async_remote_copy(
                        ref, ref, out_send.at[slot], out_recv.at[slot],
                        device_id={"ra": lax.rem(z + step, n), "cb": mate if other else cb},
                        device_id_type=MESH,
                    ))
        return made

    for copy in out_copies(False):
        copy.start()
    for side in range(2):
        @pl.when(own_side != side)
        def _():
            mix_copy(side).start()

    for side in range(2):
        mate_copy(side).wait_send()
        y_copy(side).wait_send()

        @pl.when(z != (n - 1 if side else 0))
        def _():
            sq_copy(side).wait_send()

    def drain(j, carry):
        @pl.when(z > 0)
        def _():
            rs_copy(j, 0).wait_send()
            ag_copy(j, 1).wait_send()

        @pl.when(z < n - 1)
        def _():
            rs_copy(j, 1).wait_send()
            ag_copy(j, 0).wait_send()

        return carry

    lax.fori_loop(0, chunks, drain, 0)

    for copy in out_copies(True):
        copy.wait_recv()
    total = out_all[0]
    for i in range(1, 2 * n):
        total = total + out_all[i]
    spread[...] = jnp.broadcast_to(total[:1], (128, 128)).T
    spread[...] = lax.rsqrt(spread[...] / features + EPSILON)
    out_ref[:, mine] = (mixed[...] * spread[:, :1] * ogain[:, mine]).astype(jnp.bfloat16)
    for side in range(2):
        mix_copy(side).wait_recv()
    out_ref[:, theirs] = (mixed_got[...] * spread[:, :1] * ogain[:, theirs]).astype(jnp.bfloat16)
    for side in range(2):
        mix_copy(side).wait_send()
    for copy in out_copies(False):
        copy.wait_send()


def fused(
    tokens, in_gain, gate_weight, gate_scale, up_weight, up_scale, down_weight, down_scale, out_gain
):
    n = lax.axis_size("ra")
    rows, depth = tokens.shape
    units, width = down_weight.shape
    half, blocks, chunks = rows // 2, units // WIDTH, units // SUB
    wide = width // 2
    f32, bf16 = jnp.float32, jnp.bfloat16
    vmem, dma = pltpu.VMEM, pltpu.SemaphoreType.DMA
    return pl.pallas_call(
        functools.partial(kernel, n),
        out_shape=pltpu.VMEM((rows, width), bf16),
        in_specs=[pl.BlockSpec(memory_space=pltpu.HBM)] * 9,
        out_specs=pl.BlockSpec(memory_space=pltpu.VMEM),
        scratch_shapes=[
            vmem((rows, depth), bf16), vmem((1, depth), f32),
            vmem((blocks, depth, WIDTH), f32), vmem((units // 128, 128), f32),
            vmem((blocks, depth, WIDTH), f32), vmem((units // 128, 128), f32),
            vmem((blocks, WIDTH, width), f32), vmem((1, width), f32), vmem((1, width), f32),
            vmem((rows, depth), bf16), vmem((chunks, rows, 2 * SUB), f32),
            vmem((2, chunks, half, 2 * SUB), bf16), vmem((2, chunks, half, 2 * SUB), bf16),
            vmem((2, chunks, half, SUB), bf16), vmem((2, half, width), f32),
            vmem((rows, 128), f32), vmem((8, 128), f32), vmem((2, 8, 128), f32), vmem((2, 8, 128), f32),
            vmem((rows, 128), f32),
            vmem((2, half, wide), bf16), vmem((2, half, wide), bf16),
            vmem((2, half, wide), bf16), vmem((2, half, wide), bf16),
            vmem((rows, wide), f32), vmem((rows, wide), f32), vmem((2 * n, 8, 128), f32),
            dma((6,)), dma((blocks,)), dma((blocks,)), dma((blocks,)),
            dma((2, chunks)), dma((2, chunks)), dma((2, chunks)), dma((2, chunks)),
            dma((2,)), dma((2,)), dma((2, 2)), dma((2, 2)), dma((2, 2)),
            dma((2 * n - 1,)), dma((2 * n - 1,)),
        ],
        compiler_params=pltpu.CompilerParams(
            collective_id=0, has_side_effects=True, vmem_limit_bytes=60 * 2**20
        ),
        name="fused_ffn",
    )(
        tokens, in_gain.reshape(1, -1), gate_weight, gate_scale.reshape(-1, 128), up_weight,
        up_scale.reshape(-1, 128), down_weight, down_scale.reshape(1, -1), out_gain.reshape(1, -1),
    )


def solution(mesh):
    in_specs = (
        P("grp", "ra"),
        P("ra"),
        P("ra", "cb"),
        P("cb"),
        P("ra", "cb"),
        P("cb"),
        P("cb", "ra"),
        P("ra"),
        P("ra"),
    )
    out_specs = P("grp", "ra")
    body = fused if mesh.shape["ra"] == 4 and mesh.shape["cb"] == 4 else local
    return jax.shard_map(body, mesh=mesh, in_specs=in_specs, out_specs=out_specs, check_vma=False)
```

```python
import functools
import jax
import jax.numpy as jnp
from jax import lax
from jax.experimental import pallas as pl
from jax.experimental.pallas import tpu as pltpu
from jax.sharding import PartitionSpec as P

EPSILON = 1e-06
RESIDUAL = 0.5


def local(
    tokens, in_gain, gate_weight, gate_scale, up_weight, up_scale, down_weight, down_scale, out_gain
):
    tok_float = tokens.astype(jnp.float32)
    local_squares = jnp.sum(tok_float * tok_float, axis=1)
    scaled = (tok_float * in_gain[None, :]).astype(jnp.bfloat16)
    gate_part = jnp.dot(
        scaled, gate_weight.astype(jnp.bfloat16), preferred_element_type=jnp.float32
    )
    up_part = jnp.dot(scaled, up_weight.astype(jnp.bfloat16), preferred_element_type=jnp.float32)
    features = tokens.shape[1] * lax.axis_size("ra")
    gate_sum, up_sum, share_squares = (
        lax.psum_scatter(gate_part, "ra", scatter_dimension=0, tiled=True),
        lax.psum_scatter(up_part, "ra", scatter_dimension=0, tiled=True),
        lax.psum_scatter(local_squares, "ra", scatter_dimension=0, tiled=True),
    )
    inv_rows = lax.rsqrt(share_squares / features + EPSILON)[:, None]
    gate_share = gate_sum * inv_rows * gate_scale[None, :]
    up_share = up_sum * inv_rows * up_scale[None, :]
    hidden_share = (jax.nn.silu(gate_share) * up_share).astype(jnp.bfloat16)
    hidden = lax.all_gather(hidden_share, "ra", axis=0, tiled=True)
    down_part = jnp.dot(
        hidden, down_weight.astype(jnp.bfloat16), preferred_element_type=jnp.float32
    )
    down_full = lax.psum(down_part, "cb")
    mixed_rows = RESIDUAL * tok_float + down_full * down_scale[None, :]
    out_total = lax.psum(jnp.sum(mixed_rows * mixed_rows, axis=1), "ra")
    inv_out = lax.rsqrt(out_total / features + EPSILON)[:, None]
    return (mixed_rows * inv_out * out_gain[None, :]).astype(jnp.bfloat16)


MESH = pl.DeviceIdType.MESH
WIDTH = 256
SUB = 128
AHEAD = 6
DOWN_START = 17
RS_LAG = ((22, 12, 9, 0), (0, 7, 12, 22))
AG_LAG = ((0, 28, 34, 44), (44, 34, 30, 0))
OWN_SEND = (45, 40, 42, 45)
OWN_PASS = (47, 42, 44, 47)
STEPS = 56


def pick(z, values):
    out = jnp.int32(values[0])
    for i, value in enumerate(values[1:], 1):
        out = lax.select(z == i, jnp.int32(value), out)
    return out


def kernel(
    n,
    tok_hbm, gain_hbm, gate_hbm, gscale_hbm, up_hbm, uscale_hbm, down_hbm, dscale_hbm, ogain_hbm,
    out_ref,
    tok, gain, gate, gscale, up, uscale, down, dscale, ogain,
    scaled, part, sent, got, hidden, acc, spread, sq_own, sq_sent, sq_got, inv,
    mate_sent, mate_got, y_sent, y_got, mixed, mixed_got, out_all,
    small_sem, gate_sem, up_sem, down_sem, rs_send, rs_recv, ag_send, ag_recv,
    sq_send, sq_recv, mate_sem, y_sem, mix_sem, out_sem,
):
    blocks, half = down.shape[0] // WIDTH, tok.shape[0] // 2
    chunks = part.shape[0]
    per = chunks // blocks
    rows = 2 * half
    wide = tok.shape[1] // 2
    features = tok.shape[1] * n
    z, cb = lax.axis_index("ra"), lax.axis_index("cb")
    core = lax.rem(cb, 2)
    mate = cb + 1 - 2 * core
    across = lax.rem(cb + 2, 4)
    right, left = lax.rem(z + 1, n), lax.rem(z + n - 1, n)
    own_side = (z >= n // 2).astype(jnp.int32)
    mine = pl.ds(pl.multiple_of(core * wide, wide), wide)
    theirs = pl.ds(pl.multiple_of((1 - core) * wide, wide), wide)

    smalls = [
        pltpu.make_async_copy(src, dst, small_sem.at[i])
        for i, (src, dst) in enumerate([
            (tok_hbm, tok), (gain_hbm, gain), (gscale_hbm, gscale),
            (uscale_hbm, uscale), (dscale_hbm, dscale), (ogain_hbm, ogain),
        ])
    ]

    def gate_copy(j):
        cols = pl.ds(pl.multiple_of(j * SUB, SUB), SUB)
        return pltpu.make_async_copy(gate_hbm.at[:, cols], gate.at[j], gate_sem.at[lax.rem(j, AHEAD)])

    def up_copy(j):
        cols = pl.ds(pl.multiple_of(j * SUB, SUB), SUB)
        return pltpu.make_async_copy(up_hbm.at[:, cols], up.at[j], up_sem.at[lax.rem(j, AHEAD)])

    down_copy = pltpu.make_async_copy(down_hbm, down, down_sem)

    for copy in smalls[:2]:
        copy.start()
    gate_copy(0).start()
    up_copy(0).start()

    barrier = pltpu.get_barrier_semaphore()

    @pl.when(z > 0)
    def _():
        pl.semaphore_signal(barrier, inc=1, device_id={"ra": left}, device_id_type=MESH)

    @pl.when(z < n - 1)
    def _():
        pl.semaphore_signal(barrier, inc=1, device_id={"ra": right}, device_id_type=MESH)

    for who in (mate, across):
        pl.semaphore_signal(barrier, inc=1, device_id={"cb": who}, device_id_type=MESH)

    for copy in smalls[:2]:
        copy.wait()
    for j in range(1, min(AHEAD, chunks)):
        gate_copy(j).start()
        up_copy(j).start()
    for copy in smalls[2:]:
        copy.start()
    tok_float = tok[...].astype(jnp.float32)
    scaled[...] = (tok_float * gain[...]).astype(jnp.bfloat16)
    def sq_copy(side):
        return pltpu.make_async_remote_copy(
            sq_sent.at[side], sq_got.at[side], sq_send.at[side], sq_recv.at[side],
            device_id={"ra": right if side else left}, device_id_type=MESH,
        )

    def rs_copy(j, side):
        return pltpu.make_async_remote_copy(
            sent.at[side, j], got.at[side, j], rs_send.at[side], rs_recv.at[side, j],
            device_id={"ra": right if side else left}, device_id_type=MESH,
        )

    def ag_copy(j, side):
        ref = hidden.at[side, j]
        return pltpu.make_async_remote_copy(
            ref, ref, ag_send.at[side], ag_recv.at[side, j],
            device_id={"ra": left if side else right}, device_id_type=MESH,
        )

    def rows_of(side):
        return pl.ds(side * half, half)

    def rs_step(s, side):
        place = z if side else n - 1 - z
        j = s - pick(z, RS_LAG[side])

        @pl.when((j >= 0) & (j < chunks) & (place > 0))
        def _():
            @pl.when(place < n - 1)
            def _():
                rs_copy(j, side).wait_recv()
                sent[side, j] = (part[j, rows_of(side)] + got[side, j].astype(jnp.float32)).astype(jnp.bfloat16)
                rs_copy(j, side).start()

                @pl.when(j == 0)
                def _():
                    sq_copy(side).wait_recv()
                    sq_sent[side] = sq_own[...] + sq_got[side]
                    sq_copy(side).start()

            @pl.when(place == n - 1)
            def _():
                rs_copy(j, side).wait_recv()

                @pl.when(j == 0)
                def _():
                    sq_copy(side).wait_recv()
                    total = sq_own[...] + sq_got[side]
                    spread[...] = jnp.broadcast_to(total[:1], (128, 128)).T
                    inv[...] = lax.rsqrt(spread[...] / features + EPSILON)

                scale = inv[rows_of(side)]
                total = part[j, rows_of(side)] + got[side, j].astype(jnp.float32)
                gate_share = total[:, :SUB] * scale * gscale[pl.ds(j, 1)]
                up_share = total[:, SUB:] * scale * uscale[pl.ds(j, 1)]
                hidden[side, j] = (jax.nn.silu(gate_share) * up_share).astype(jnp.bfloat16)
                ag_copy(j, side).start()

    def ag_step(s, side, i):
        place = n - 1 - z if side else z
        j = per * (s - pick(z, AG_LAG[side])) + i

        @pl.when((j >= 0) & (j < chunks) & (place > 0))
        def _():
            ag_copy(j, side).wait_recv()

            @pl.when(place < n - 1)
            def _():
                ag_copy(j, side).start()

    def down_step(s, side):
        place = n - 1 - z if side else z
        since = s - pick(z, RS_LAG[side])
        k = lax.select(place > 0, s - pick(z, AG_LAG[side]), since // per)

        @pl.when((k >= 0) & (k < blocks) & ((place > 0) | (lax.rem(since, per) == per - 1)))
        def _():
            units = jnp.concatenate([hidden[side, per * k + i] for i in range(per)], axis=1)
            weights = down[pl.ds(pl.multiple_of(k * WIDTH, WIDTH), WIDTH)].astype(jnp.bfloat16)
            acc[side] += jnp.dot(units, weights, preferred_element_type=jnp.float32)

    def mate_copy(side):
        return pltpu.make_async_remote_copy(
            mate_sent.at[side], mate_got.at[side], mate_sem.at[0, side], mate_sem.at[1, side],
            device_id={"cb": mate}, device_id_type=MESH,
        )

    def y_copy(side):
        return pltpu.make_async_remote_copy(
            y_sent.at[side], y_got.at[side], y_sem.at[0, side], y_sem.at[1, side],
            device_id={"cb": across}, device_id_type=MESH,
        )

    def mix_copy(side):
        at = rows_of(side)
        return pltpu.make_async_remote_copy(
            mixed.at[at], mixed_got.at[at], mix_sem.at[0, side], mix_sem.at[1, side],
            device_id={"cb": mate}, device_id_type=MESH,
        )

    def mate_start(side):
        mate_sent[side] = acc[side, :, theirs].astype(jnp.bfloat16)
        mate_copy(side).start()

    def y_start(side):
        mate_copy(side).wait_recv()
        y_sent[side] = (acc[side, :, mine] + mate_got[side].astype(jnp.float32)).astype(jnp.bfloat16)
        y_copy(side).start()

    def mix_start(side):
        y_copy(side).wait_recv()
        at = rows_of(side)
        summed = y_sent[side].astype(jnp.float32) + y_got[side].astype(jnp.float32)
        value = RESIDUAL * tok[at, mine].astype(jnp.float32) + summed * dscale[:, mine]
        mixed[at] = value
        spread[at] = jnp.broadcast_to(jnp.sum(value * value, axis=1, keepdims=True), (half, 128))

    def first(side):
        return z == (0 if side else n - 1)

    def dot_step(j):
        gate_copy(j).wait()
        up_copy(j).wait()
        weights = jnp.concatenate([gate[j], up[j]], axis=1).astype(jnp.bfloat16)
        part[j] = jnp.dot(scaled[...], weights, preferred_element_type=jnp.float32)

    def send_step(j, side):
        @pl.when(first(side))
        def _():
            sent[side, j] = part[j, rows_of(side)].astype(jnp.bfloat16)
            rs_copy(j, side).start()

    dot_step(0)
    pl.semaphore_wait(barrier, 2 + (z > 0).astype(jnp.int32) + (z < n - 1).astype(jnp.int32))
    for side in range(2):
        send_step(0, side)
    tok_float = tok[...].astype(jnp.float32)
    squares = jnp.sum(tok_float * tok_float, axis=1, keepdims=True)
    spread[...] = jnp.broadcast_to(squares, (rows, 128))
    sq_own[...] = spread[...].T[:8]
    for side in range(2):
        @pl.when(first(side))
        def _():
            sq_sent[side] = sq_own[...]
            sq_copy(side).start()

    gate_copy(AHEAD).start()
    up_copy(AHEAD).start()

    def dots(s, carry):
        for side in (1, 0):
            rs_step(s, side)
        dot_step(s)
        for side in range(2):
            send_step(s, side)

        @pl.when(s + AHEAD < chunks)
        def _():
            gate_copy(s + AHEAD).start()
            up_copy(s + AHEAD).start()

        @pl.when(s == DOWN_START)
        def _():
            down_copy.start()

        return carry

    lax.fori_loop(1, chunks, dots, 0)
    for copy in smalls[2:]:
        copy.wait()
    for side in range(2):
        acc[side] = jnp.zeros_like(acc[side])

    def gathers(s):
        for i in range(per):
            for side in range(2):
                ag_step(s, side, i)
        for side in range(2):
            down_step(s, side)
        for side in range(2):
            @pl.when(own_side == side)
            def _():
                @pl.when(s == pick(z, OWN_SEND))
                def _():
                    mate_start(side)

                @pl.when(s == pick(z, OWN_PASS))
                def _():
                    y_start(side)

    def sums(s, carry):
        for side in (1, 0):
            rs_step(s, side)

        @pl.when(s == chunks + 1)
        def _():
            down_copy.wait()

        gathers(s)
        return carry

    def rest(s, carry):
        gathers(s)
        return carry

    lax.fori_loop(chunks, 2 * chunks, sums, 0)
    lax.fori_loop(2 * chunks, STEPS, rest, 0)

    for side in range(2):
        @pl.when(own_side != side)
        def _():
            mate_start(side)
            mix_start(1 - side)
            mix_copy(1 - side).start()
            y_start(side)
            mix_start(side)

    at = 2 * z + core
    out_all[at] = spread[...].T[:8]

    for step in range(n):
        for other in range(2):
            if step or other:
                pltpu.make_async_remote_copy(
                    out_all.at[at], out_all.at[at], out_sem.at[0], out_sem.at[1],
                    device_id={"ra": lax.rem(z + step, n), "cb": mate if other else cb},
                    device_id_type=MESH,
                ).start()
    out_copies = pltpu.make_async_remote_copy(
        out_all.at[pl.ds(0, 2 * n - 1)], out_all.at[pl.ds(0, 2 * n - 1)], out_sem.at[0], out_sem.at[1],
        device_id={"cb": mate}, device_id_type=MESH,
    )
    for side in range(2):
        @pl.when(own_side != side)
        def _():
            mix_copy(side).start()

    for side in range(2):
        mate_copy(side).wait_send()
        y_copy(side).wait_send()

        @pl.when(z != (n - 1 if side else 0))
        def _():
            sq_copy(side).wait_send()

    def drain(side):
        pltpu.make_async_remote_copy(
            sent.at[side], got.at[side], rs_send.at[side], rs_recv.at[side, 0],
            device_id={"ra": right if side else left}, device_id_type=MESH,
        ).wait_send()
        pltpu.make_async_remote_copy(
            hidden.at[1 - side], hidden.at[1 - side], ag_send.at[1 - side], ag_recv.at[1 - side, 0],
            device_id={"ra": right if side else left}, device_id_type=MESH,
        ).wait_send()

    for side in range(2):
        @pl.when(z != (n - 1 if side else 0))
        def _():
            drain(side)

    out_copies.wait_recv()
    total = out_all[0]
    for i in range(1, 2 * n):
        total = total + out_all[i]
    spread[...] = jnp.broadcast_to(total[:1], (128, 128)).T
    spread[...] = lax.rsqrt(spread[...] / features + EPSILON)
    out_ref[:, mine] = (mixed[...] * spread[:, :1] * ogain[:, mine]).astype(jnp.bfloat16)
    for side in range(2):
        mix_copy(side).wait_recv()
    out_ref[:, theirs] = (mixed_got[...] * spread[:, :1] * ogain[:, theirs]).astype(jnp.bfloat16)
    for side in range(2):
        mix_copy(side).wait_send()
    out_copies.wait_send()


def fused(
    tokens, in_gain, gate_weight, gate_scale, up_weight, up_scale, down_weight, down_scale, out_gain
):
    n = lax.axis_size("ra")
    rows, depth = tokens.shape
    units, width = down_weight.shape
    half, blocks, chunks = rows // 2, units // WIDTH, units // SUB
    wide = width // 2
    f32, bf16 = jnp.float32, jnp.bfloat16
    vmem, dma = pltpu.VMEM, pltpu.SemaphoreType.DMA
    return pl.pallas_call(
        functools.partial(kernel, n),
        out_shape=pltpu.VMEM((rows, width), bf16),
        in_specs=[pl.BlockSpec(memory_space=pltpu.HBM)] * 9,
        out_specs=pl.BlockSpec(memory_space=pltpu.VMEM),
        scratch_shapes=[
            vmem((rows, depth), bf16), vmem((1, depth), f32),
            vmem((chunks, depth, SUB), f32), vmem((units // 128, 128), f32),
            vmem((chunks, depth, SUB), f32), vmem((units // 128, 128), f32),
            vmem((units, width), f32), vmem((1, width), f32), vmem((1, width), f32),
            vmem((rows, depth), bf16), vmem((chunks, rows, 2 * SUB), f32),
            vmem((2, chunks, half, 2 * SUB), bf16), vmem((2, chunks, half, 2 * SUB), bf16),
            vmem((2, chunks, half, SUB), bf16), vmem((2, half, width), f32),
            vmem((rows, 128), f32), vmem((8, 128), f32), vmem((2, 8, 128), f32), vmem((2, 8, 128), f32),
            vmem((rows, 128), f32),
            vmem((2, half, wide), bf16), vmem((2, half, wide), bf16),
            vmem((2, half, wide), bf16), vmem((2, half, wide), bf16),
            vmem((rows, wide), f32), vmem((rows, wide), f32), vmem((2 * n, 8, 128), f32),
            dma((6,)), dma((AHEAD,)), dma((AHEAD,)), dma,
            dma((2,)), dma((2, chunks)), dma((2,)), dma((2, chunks)),
            dma((2,)), dma((2,)), dma((2, 2)), dma((2, 2)), dma((2, 2)), dma((2,)),
        ],
        compiler_params=pltpu.CompilerParams(
            collective_id=0, has_side_effects=True, vmem_limit_bytes=60 * 2**20
        ),
        name="fused_ffn",
    )(
        tokens, in_gain.reshape(1, -1), gate_weight, gate_scale.reshape(-1, 128), up_weight,
        up_scale.reshape(-1, 128), down_weight, down_scale.reshape(1, -1), out_gain.reshape(1, -1),
    )


def solution(mesh):
    in_specs = (
        P("grp", "ra"),
        P("ra"),
        P("ra", "cb"),
        P("cb"),
        P("ra", "cb"),
        P("cb"),
        P("cb", "ra"),
        P("ra"),
        P("ra"),
    )
    out_specs = P("grp", "ra")
    body = fused if mesh.shape["ra"] == 4 and mesh.shape["cb"] == 4 else local
    return jax.shard_map(body, mesh=mesh, in_specs=in_specs, out_specs=out_specs, check_vma=False)
```

```python
import functools
import jax
import jax.numpy as jnp
from jax import lax
from jax.experimental import pallas as pl
from jax.experimental.pallas import tpu as pltpu
from jax.sharding import PartitionSpec as P

EPSILON = 1e-06
RESIDUAL = 0.5


def local(
    tokens, in_gain, gate_weight, gate_scale, up_weight, up_scale, down_weight, down_scale, out_gain
):
    tok_float = tokens.astype(jnp.float32)
    local_squares = jnp.sum(tok_float * tok_float, axis=1)
    scaled = (tok_float * in_gain[None, :]).astype(jnp.bfloat16)
    gate_part = jnp.dot(
        scaled, gate_weight.astype(jnp.bfloat16), preferred_element_type=jnp.float32
    )
    up_part = jnp.dot(scaled, up_weight.astype(jnp.bfloat16), preferred_element_type=jnp.float32)
    features = tokens.shape[1] * lax.axis_size("ra")
    gate_sum, up_sum, share_squares = (
        lax.psum_scatter(gate_part, "ra", scatter_dimension=0, tiled=True),
        lax.psum_scatter(up_part, "ra", scatter_dimension=0, tiled=True),
        lax.psum_scatter(local_squares, "ra", scatter_dimension=0, tiled=True),
    )
    inv_rows = lax.rsqrt(share_squares / features + EPSILON)[:, None]
    gate_share = gate_sum * inv_rows * gate_scale[None, :]
    up_share = up_sum * inv_rows * up_scale[None, :]
    hidden_share = (jax.nn.silu(gate_share) * up_share).astype(jnp.bfloat16)
    hidden = lax.all_gather(hidden_share, "ra", axis=0, tiled=True)
    down_part = jnp.dot(
        hidden, down_weight.astype(jnp.bfloat16), preferred_element_type=jnp.float32
    )
    down_full = lax.psum(down_part, "cb")
    mixed_rows = RESIDUAL * tok_float + down_full * down_scale[None, :]
    out_total = lax.psum(jnp.sum(mixed_rows * mixed_rows, axis=1), "ra")
    inv_out = lax.rsqrt(out_total / features + EPSILON)[:, None]
    return (mixed_rows * inv_out * out_gain[None, :]).astype(jnp.bfloat16)


MESH = pl.DeviceIdType.MESH
WIDTH = 256
SUB = 128
AHEAD = 6
DOWN_START = 8
RS_LAG = ((22, 12, 9, 0), (0, 7, 12, 22))
AG_LAG = ((0, 28, 34, 44), (44, 34, 30, 0))
OWN_SEND = (45, 40, 42, 45)
OWN_PASS = (47, 42, 44, 47)
STEPS = 56


def pick(z, values):
    out = jnp.int32(values[0])
    for i, value in enumerate(values[1:], 1):
        out = lax.select(z == i, jnp.int32(value), out)
    return out


def kernel(
    n,
    tok_hbm, gain_hbm, gate_hbm, gscale_hbm, up_hbm, uscale_hbm, down_hbm, dscale_hbm, ogain_hbm,
    out_ref,
    tok, gain, gate, gscale, up, uscale, down, dscale, ogain,
    scaled, part, sent, got, hidden, acc, spread, sq_own, sq_sent, sq_got, inv,
    mate_sent, mate_got, y_sent, y_got, mixed, mixed_got, out_all,
    small_sem, gate_sem, up_sem, down_sem, rs_send, rs_recv, ag_send, ag_recv,
    sq_send, sq_recv, mate_sem, y_sem, mix_sem, out_sem,
):
    blocks, half = down.shape[0] // WIDTH, tok.shape[0] // 2
    chunks = part.shape[0]
    per = chunks // blocks
    rows = 2 * half
    wide = tok.shape[1] // 2
    features = tok.shape[1] * n
    z, cb = lax.axis_index("ra"), lax.axis_index("cb")
    core = lax.rem(cb, 2)
    mate = cb + 1 - 2 * core
    across = lax.rem(cb + 2, 4)
    right, left = lax.rem(z + 1, n), lax.rem(z + n - 1, n)
    own_side = (z >= n // 2).astype(jnp.int32)
    mine = pl.ds(pl.multiple_of(core * wide, wide), wide)
    theirs = pl.ds(pl.multiple_of((1 - core) * wide, wide), wide)

    smalls = [
        pltpu.make_async_copy(src, dst, small_sem.at[i])
        for i, (src, dst) in enumerate([
            (tok_hbm, tok), (gain_hbm, gain), (gscale_hbm, gscale),
            (uscale_hbm, uscale), (dscale_hbm, dscale), (ogain_hbm, ogain),
        ])
    ]

    def gate_copy(j):
        cols = pl.ds(pl.multiple_of(j * SUB, SUB), SUB)
        return pltpu.make_async_copy(gate_hbm.at[:, cols], gate.at[j], gate_sem.at[lax.rem(j, AHEAD)])

    def up_copy(j):
        cols = pl.ds(pl.multiple_of(j * SUB, SUB), SUB)
        return pltpu.make_async_copy(up_hbm.at[:, cols], up.at[j], up_sem.at[lax.rem(j, AHEAD)])

    def down_copy(k):
        at = pl.ds(pl.multiple_of(k * WIDTH, WIDTH), WIDTH)
        return pltpu.make_async_copy(down_hbm.at[at], down.at[at], down_sem)

    for copy in smalls[:2]:
        copy.start()
    gate_copy(0).start()
    up_copy(0).start()

    barrier = pltpu.get_barrier_semaphore()

    @pl.when(z > 0)
    def _():
        pl.semaphore_signal(barrier, inc=1, device_id={"ra": left}, device_id_type=MESH)

    @pl.when(z < n - 1)
    def _():
        pl.semaphore_signal(barrier, inc=1, device_id={"ra": right}, device_id_type=MESH)

    for who in (mate, across):
        pl.semaphore_signal(barrier, inc=1, device_id={"cb": who}, device_id_type=MESH)

    for copy in smalls[:2]:
        copy.wait()
    for j in range(1, min(AHEAD, chunks)):
        gate_copy(j).start()
        up_copy(j).start()
    for copy in smalls[2:]:
        copy.start()
    tok_float = tok[...].astype(jnp.float32)
    scaled[...] = (tok_float * gain[...]).astype(jnp.bfloat16)
    def sq_copy(side):
        return pltpu.make_async_remote_copy(
            sq_sent.at[side], sq_got.at[side], sq_send.at[side], sq_recv.at[side],
            device_id={"ra": right if side else left}, device_id_type=MESH,
        )

    def rs_copy(j, side):
        return pltpu.make_async_remote_copy(
            sent.at[side, j], got.at[side, j], rs_send.at[side], rs_recv.at[side, j],
            device_id={"ra": right if side else left}, device_id_type=MESH,
        )

    def ag_copy(j, side):
        ref = hidden.at[side, j]
        return pltpu.make_async_remote_copy(
            ref, ref, ag_send.at[side], ag_recv.at[side, j],
            device_id={"ra": left if side else right}, device_id_type=MESH,
        )

    def rows_of(side):
        return pl.ds(side * half, half)

    def rs_step(s, side):
        place = z if side else n - 1 - z
        j = s - pick(z, RS_LAG[side])

        @pl.when((j >= 0) & (j < chunks) & (place > 0))
        def _():
            @pl.when(place < n - 1)
            def _():
                rs_copy(j, side).wait_recv()
                sent[side, j] = (part[j, rows_of(side)] + got[side, j].astype(jnp.float32)).astype(jnp.bfloat16)
                rs_copy(j, side).start()

                @pl.when(j == 0)
                def _():
                    sq_copy(side).wait_recv()
                    sq_sent[side] = sq_own[...] + sq_got[side]
                    sq_copy(side).start()

            @pl.when(place == n - 1)
            def _():
                rs_copy(j, side).wait_recv()

                @pl.when(j == 0)
                def _():
                    sq_copy(side).wait_recv()
                    total = sq_own[...] + sq_got[side]
                    spread[...] = jnp.broadcast_to(total[:1], (128, 128)).T
                    inv[...] = lax.rsqrt(spread[...] / features + EPSILON)

                scale = inv[rows_of(side)]
                total = part[j, rows_of(side)] + got[side, j].astype(jnp.float32)
                gate_share = total[:, :SUB] * scale * gscale[pl.ds(j, 1)]
                up_share = total[:, SUB:] * scale * uscale[pl.ds(j, 1)]
                hidden[side, j] = (jax.nn.silu(gate_share) * up_share).astype(jnp.bfloat16)
                ag_copy(j, side).start()

    def ag_step(s, side, i):
        place = n - 1 - z if side else z
        j = per * (s - pick(z, AG_LAG[side])) + i

        @pl.when((j >= 0) & (j < chunks) & (place > 0))
        def _():
            ag_copy(j, side).wait_recv()

            @pl.when(place < n - 1)
            def _():
                ag_copy(j, side).start()

    def down_step(s, side):
        place = n - 1 - z if side else z
        since = s - pick(z, RS_LAG[side])
        k = lax.select(place > 0, s - pick(z, AG_LAG[side]), since // per)

        @pl.when((k >= 0) & (k < blocks) & ((place > 0) | (lax.rem(since, per) == per - 1)))
        def _():
            units = jnp.concatenate([hidden[side, per * k + i] for i in range(per)], axis=1)
            weights = down[pl.ds(pl.multiple_of(k * WIDTH, WIDTH), WIDTH)].astype(jnp.bfloat16)
            acc[side] += jnp.dot(units, weights, preferred_element_type=jnp.float32)

    def mate_copy(side):
        return pltpu.make_async_remote_copy(
            mate_sent.at[side], mate_got.at[side], mate_sem.at[0, side], mate_sem.at[1, side],
            device_id={"cb": mate}, device_id_type=MESH,
        )

    def y_copy(side):
        return pltpu.make_async_remote_copy(
            y_sent.at[side], y_got.at[side], y_sem.at[0, side], y_sem.at[1, side],
            device_id={"cb": across}, device_id_type=MESH,
        )

    def mix_copy(side):
        at = rows_of(side)
        return pltpu.make_async_remote_copy(
            mixed.at[at], mixed_got.at[at], mix_sem.at[0, side], mix_sem.at[1, side],
            device_id={"cb": mate}, device_id_type=MESH,
        )

    def mate_start(side):
        mate_sent[side] = acc[side, :, theirs].astype(jnp.bfloat16)
        mate_copy(side).start()

    def y_start(side):
        mate_copy(side).wait_recv()
        y_sent[side] = (acc[side, :, mine] + mate_got[side].astype(jnp.float32)).astype(jnp.bfloat16)
        y_copy(side).start()

    def mix_start(side):
        y_copy(side).wait_recv()
        at = rows_of(side)
        summed = y_sent[side].astype(jnp.float32) + y_got[side].astype(jnp.float32)
        value = RESIDUAL * tok[at, mine].astype(jnp.float32) + summed * dscale[:, mine]
        mixed[at] = value
        spread[at] = jnp.broadcast_to(jnp.sum(value * value, axis=1, keepdims=True), (half, 128))

    def first(side):
        return z == (0 if side else n - 1)

    def dot_step(j):
        gate_copy(j).wait()
        up_copy(j).wait()
        weights = jnp.concatenate([gate[j], up[j]], axis=1).astype(jnp.bfloat16)
        part[j] = jnp.dot(scaled[...], weights, preferred_element_type=jnp.float32)

    def send_step(j, side):
        @pl.when(first(side))
        def _():
            sent[side, j] = part[j, rows_of(side)].astype(jnp.bfloat16)
            rs_copy(j, side).start()

    dot_step(0)
    pl.semaphore_wait(barrier, 2 + (z > 0).astype(jnp.int32) + (z < n - 1).astype(jnp.int32))
    for side in range(2):
        send_step(0, side)
    tok_float = tok[...].astype(jnp.float32)
    squares = jnp.sum(tok_float * tok_float, axis=1, keepdims=True)
    spread[...] = jnp.broadcast_to(squares, (rows, 128))
    sq_own[...] = spread[...].T[:8]
    for side in range(2):
        @pl.when(first(side))
        def _():
            sq_sent[side] = sq_own[...]
            sq_copy(side).start()

    gate_copy(AHEAD).start()
    up_copy(AHEAD).start()

    def dots(s, carry):
        for side in (0, 1):
            rs_step(s, side)
        dot_step(s)
        for side in range(2):
            send_step(s, side)

        @pl.when(s + AHEAD < chunks)
        def _():
            gate_copy(s + AHEAD).start()
            up_copy(s + AHEAD).start()

        @pl.when((s >= DOWN_START) & (s < DOWN_START + blocks))
        def _():
            down_copy(s - DOWN_START).start()

        return carry

    lax.fori_loop(1, chunks, dots, 0)
    for copy in smalls[2:]:
        copy.wait()
    for side in range(2):
        acc[side] = jnp.zeros_like(acc[side])

    def gathers(s):
        for i in range(per):
            for side in range(2):
                ag_step(s, side, i)
        for side in range(2):
            down_step(s, side)
        for side in range(2):
            @pl.when(own_side == side)
            def _():
                @pl.when(s == pick(z, OWN_SEND))
                def _():
                    mate_start(side)

                @pl.when(s == pick(z, OWN_PASS))
                def _():
                    y_start(side)

    def sums(s, carry):
        for side in (0, 1):
            rs_step(s, side)

        @pl.when(s == chunks + 1)
        def _():
            pltpu.make_async_copy(down_hbm, down, down_sem).wait()

        gathers(s)
        return carry

    def rest(s, carry):
        gathers(s)
        return carry

    lax.fori_loop(chunks, 2 * chunks, sums, 0)
    lax.fori_loop(2 * chunks, STEPS, rest, 0)

    for side in range(2):
        @pl.when(own_side != side)
        def _():
            mate_start(side)
            mix_start(1 - side)
            mix_copy(1 - side).start()
            y_start(side)
            mix_start(side)

    at = 2 * z + core
    out_all[at] = spread[...].T[:8]

    for step in range(n):
        for other in range(2):
            if step or other:
                pltpu.make_async_remote_copy(
                    out_all.at[at], out_all.at[at], out_sem.at[0], out_sem.at[1],
                    device_id={"ra": lax.rem(z + step, n), "cb": mate if other else cb},
                    device_id_type=MESH,
                ).start()
    out_copies = pltpu.make_async_remote_copy(
        out_all.at[pl.ds(0, 2 * n - 1)], out_all.at[pl.ds(0, 2 * n - 1)], out_sem.at[0], out_sem.at[1],
        device_id={"cb": mate}, device_id_type=MESH,
    )
    for side in range(2):
        @pl.when(own_side != side)
        def _():
            mix_copy(side).start()

    for side in range(2):
        mate_copy(side).wait_send()
        y_copy(side).wait_send()

        @pl.when(z != (n - 1 if side else 0))
        def _():
            sq_copy(side).wait_send()

    def drain(side):
        pltpu.make_async_remote_copy(
            sent.at[side], got.at[side], rs_send.at[side], rs_recv.at[side, 0],
            device_id={"ra": right if side else left}, device_id_type=MESH,
        ).wait_send()
        pltpu.make_async_remote_copy(
            hidden.at[1 - side], hidden.at[1 - side], ag_send.at[1 - side], ag_recv.at[1 - side, 0],
            device_id={"ra": right if side else left}, device_id_type=MESH,
        ).wait_send()

    for side in range(2):
        @pl.when(z != (n - 1 if side else 0))
        def _():
            drain(side)

    out_copies.wait_recv()
    total = out_all[0]
    for i in range(1, 2 * n):
        total = total + out_all[i]
    spread[...] = jnp.broadcast_to(total[:1], (128, 128)).T
    spread[...] = lax.rsqrt(spread[...] / features + EPSILON)
    out_ref[:, mine] = (mixed[...] * spread[:, :1] * ogain[:, mine]).astype(jnp.bfloat16)
    for side in range(2):
        mix_copy(side).wait_recv()
    out_ref[:, theirs] = (mixed_got[...] * spread[:, :1] * ogain[:, theirs]).astype(jnp.bfloat16)
    for side in range(2):
        mix_copy(side).wait_send()
    out_copies.wait_send()


def fused(
    tokens, in_gain, gate_weight, gate_scale, up_weight, up_scale, down_weight, down_scale, out_gain
):
    n = lax.axis_size("ra")
    rows, depth = tokens.shape
    units, width = down_weight.shape
    half, blocks, chunks = rows // 2, units // WIDTH, units // SUB
    wide = width // 2
    f32, bf16 = jnp.float32, jnp.bfloat16
    vmem, dma = pltpu.VMEM, pltpu.SemaphoreType.DMA
    return pl.pallas_call(
        functools.partial(kernel, n),
        out_shape=pltpu.VMEM((rows, width), bf16),
        in_specs=[pl.BlockSpec(memory_space=pltpu.HBM)] * 9,
        out_specs=pl.BlockSpec(memory_space=pltpu.VMEM),
        scratch_shapes=[
            vmem((rows, depth), bf16), vmem((1, depth), f32),
            vmem((chunks, depth, SUB), f32), vmem((units // 128, 128), f32),
            vmem((chunks, depth, SUB), f32), vmem((units // 128, 128), f32),
            vmem((units, width), f32), vmem((1, width), f32), vmem((1, width), f32),
            vmem((rows, depth), bf16), vmem((chunks, rows, 2 * SUB), f32),
            vmem((2, chunks, half, 2 * SUB), bf16), vmem((2, chunks, half, 2 * SUB), bf16),
            vmem((2, chunks, half, SUB), bf16), vmem((2, half, width), f32),
            vmem((rows, 128), f32), vmem((8, 128), f32), vmem((2, 8, 128), f32), vmem((2, 8, 128), f32),
            vmem((rows, 128), f32),
            vmem((2, half, wide), bf16), vmem((2, half, wide), bf16),
            vmem((2, half, wide), bf16), vmem((2, half, wide), bf16),
            vmem((rows, wide), f32), vmem((rows, wide), f32), vmem((2 * n, 8, 128), f32),
            dma((6,)), dma((AHEAD,)), dma((AHEAD,)), dma,
            dma((2,)), dma((2, chunks)), dma((2,)), dma((2, chunks)),
            dma((2,)), dma((2,)), dma((2, 2)), dma((2, 2)), dma((2, 2)), dma((2,)),
        ],
        compiler_params=pltpu.CompilerParams(
            collective_id=0, has_side_effects=True, vmem_limit_bytes=60 * 2**20
        ),
        name="fused_ffn",
    )(
        tokens, in_gain.reshape(1, -1), gate_weight, gate_scale.reshape(-1, 128), up_weight,
        up_scale.reshape(-1, 128), down_weight, down_scale.reshape(1, -1), out_gain.reshape(1, -1),
    )


def solution(mesh):
    in_specs = (
        P("grp", "ra"),
        P("ra"),
        P("ra", "cb"),
        P("cb"),
        P("ra", "cb"),
        P("cb"),
        P("cb", "ra"),
        P("ra"),
        P("ra"),
    )
    out_specs = P("grp", "ra")
    body = fused if mesh.shape["ra"] == 4 and mesh.shape["cb"] == 4 else local
    return jax.shard_map(body, mesh=mesh, in_specs=in_specs, out_specs=out_specs, check_vma=False)
```
